256 devices in a mesh: ep: 16 (over y, x), tp: 16 (over z, core).
Axes of the slice: x: 4, y: 4, z: 8, core: 2. Of those that a mesh axis runs over, the one named last changes fastest.
Arguments:
- layer_in: bfloat16 [512, 2048], P('ep'), may hold values from -6 to 6
- attn_gain: float32 [2048], replicated, may hold values from 0.1 to 1.9
- query_weight: bfloat16 [2048, 1024], P(None, 'tp'), may hold values from -0.125 to 0.125
- key_weight: bfloat16 [2048, 1024], P(None, 'tp'), may hold values from -0.125 to 0.125
- value_weight: bfloat16 [2048, 1024], P(None, 'tp'), may hold values from -0.125 to 0.125
- forget_weight: bfloat16 [2048, 16], replicated, may hold values from -0.125 to 0.125
- forget_bias: float32 [16], replicated, may hold values from -2 to 3
- out_weight: bfloat16 [1024, 2048], P('tp'), may hold values from -0.1875 to 0.1875
- kv_cache: bfloat16 [512, 16, 1024, 128], P('ep', 'tp'), may hold values from -110 to 110
- cum_gates: float32 [512, 16, 1024], P('ep', 'tp'), may hold values from -144 to 0, as said below
- lengths: int32 [512], P('ep'), may hold values from 512 to 1024, as said below
- ffn_gain: float32 [2048], replicated, may hold values from 0.1 to 1.9
- route_ids: int32 [512, 6], P('ep'), may hold values from 0 to 127, all different within a row; in each aligned block of 32 rows (0 to 31, 32 to 63, ...) at most 2 rows name the same one
- route_weights: float32 [512, 6], P('ep'), may hold values from 0.1 to 1
- shared_gate: bfloat16 [2048, 512], P(None, 'tp'), may hold values from -0.125 to 0.125
- shared_up: bfloat16 [2048, 512], P(None, 'tp'), may hold values from -0.125 to 0.125
- shared_down: bfloat16 [512, 2048], P('tp'), may hold values from -0.25 to 0.25
- expert_gate: bfloat16 [256, 2048, 256], P(('ep', 'tp')), may hold values from -0.125 to 0.125
- expert_up: bfloat16 [256, 2048, 256], P(('ep', 'tp')), may hold values from -0.125 to 0.125
- expert_down: bfloat16 [256, 256, 2048], P(('ep', 'tp')), may hold values from -0.25 to 0.25
Outputs:
- layer_out: bfloat16 [512, 2048], P('ep')
- new_kv: bfloat16 [512, 16, 128], P('ep', 'tp')
The draws below stay inside these ranges and needn't reach their ends.
Inputs may be any that keep to these rules, and one draw needn't show every extreme that they name: `cum_gates`: never rising along positions. `lengths`: every length is at most 1024, and some sequence's length is exactly 1024. `route_ids`: each row names 6 different experts. Among the 32 rows of one index of ep (aligned blocks), no expert is named by more than 2 rows, and in some block one expert is named by exactly 2 rows.
All inputs are finite; a program needn't handle non-finite values.
Results may differ from the reference program's by a relative error of at most 0.019.
Values may be sent and summed in bfloat16 or wider, within the bound.
A program may use at most 64 MiB of HBM per device.

```python
import math
import jax
import jax.numpy as jnp
import numpy as np
from jax import lax

D = 2048
HEADS = 16
HD = 64
EFF = 512
SFF = 512
TOPK = 6
SEQ_GRP = 32
CACHE_LENGTH = 1024
SEQS = 512
EXPERTS = 128
CAP = 2
N_EP = 16


def draw_kv_cache(key, part):
    tensor_extent = (SEQS, HEADS, CACHE_LENGTH, 2 * HD)
    base = jnp.clip(jax.random.normal(key, tensor_extent, jnp.float32), -6.0, 6.0)
    return base.astype(jnp.bfloat16)


def draw_cum_gates(key, part):
    tensor_extent = (SEQS, HEADS, CACHE_LENGTH)
    slow_share = 0.5
    slow = jax.random.bernoulli(jax.random.fold_in(key, 1), slow_share, (1, HEADS, 1))
    decay_rates = jnp.where(slow, 0.5 / CACHE_LENGTH, 1.0 / 40.0)
    sequence_multiplier = jnp.exp(jax.random.uniform(jax.random.fold_in(key, 2), (SEQS, 1, 1), jnp.float32, -0.7, 0.7))
    approximate_value = jnp.exp(jax.random.uniform(jax.random.fold_in(key, 3), tensor_extent, jnp.float32, -0.7, 0.7))
    spike_position = jax.random.bernoulli(jax.random.fold_in(key, 4), 2.0 / CACHE_LENGTH, tensor_extent)
    spike_length = jax.random.uniform(jax.random.fold_in(key, 5), tensor_extent, jnp.float32, 0.22, 0.69)
    decode_iterations = decay_rates * sequence_multiplier * approximate_value + jnp.where(spike_position, spike_length, 0.0)
    return jnp.cumsum(-decode_iterations, axis=-1)


def draw_lengths(key, part):
    drawn = jax.random.randint(key, (SEQS,), CACHE_LENGTH // 2, CACHE_LENGTH + 1, dtype=jnp.int32)
    return drawn.at[0].set(CACHE_LENGTH)


def block_levels(stream_key, extent, shards, low, top_value):
    def one(dim, shards_of):
        draws = jax.random.uniform(jax.random.fold_in(jax.random.fold_in(stream_key, 6), dim), (shards_of,), jnp.float32, low / len(shards), top_value / len(shards))
        return jnp.repeat(jnp.exp(draws), extent[dim] // shards_of).reshape((-1,) + (1,) * (len(extent) - dim - 1))

    level = one(*shards[0])
    for cut in shards[1:]:
        level = level * one(*cut)
    return level


def deal_out(rng, own, number, rows, amount, top, reach, lean):
    order = jax.random.permutation(rng, amount)
    crowded, ordinary = load_shares(amount, rows * top, reach, lean, True), load_shares(amount, rows * top, reach, lean, False)
    places = jnp.arange(amount)

    def named(sizes, turn):
        used = int((sizes > 0).sum())
        fixed = max(1, used // 4)
        moved = fixed + (places - fixed + turn * (used - fixed)) % max(1, amount - fixed)
        return jnp.zeros((amount,), jnp.int32).at[order[jnp.where(places < fixed, places, moved)]].set(jnp.asarray(sizes, jnp.int32))

    sizes = jnp.where(number % 4 == 0, named(crowded, number // 4), named(ordinary, number - number // 4 - 1))
    mixed = jax.random.permutation(jax.random.fold_in(own, 3), amount)
    donor, receiver = mixed[0:amount // 2 * 2:2], mixed[1:amount // 2 * 2:2]
    margin = jnp.minimum(sizes[donor] - 1, reach - sizes[receiver]) // 2
    margin = jnp.where((donor == order[0]) | (receiver == order[0]) | (sizes[receiver] == 0), 0, jnp.maximum(margin, 0))
    moved = jax.random.randint(jax.random.fold_in(own, 4), (amount // 2,), 0, 1 << 20) % (margin + 1)
    sizes = sizes.at[donor].add(-moved).at[receiver].add(moved)
    items = jnp.searchsorted(jnp.cumsum(sizes), jnp.arange(rows * top), side="right").astype(jnp.int32)
    listing = items.reshape(top, rows).T
    listing = listing[jax.random.permutation(jax.random.fold_in(own, 1), rows)]
    turn = jax.random.randint(jax.random.fold_in(own, 2), (rows, 1), 0, top)
    return jnp.take_along_axis(listing, (jnp.arange(top)[None, :] + turn) % top, axis=1)


def load_shares(amount, total, reach, slope, full):
    portions = [(1 << 20) // math.isqrt(rank ** slope) + 1 for rank in range(1, amount + 1)]
    largest = reach if full else min(reach, max(-(-total // amount), total * portions[0] // sum(portions)))
    least = 1 if total - largest >= amount - 1 else 0
    given, spare = [largest] + [least] * (amount - 1), total - largest - least * (amount - 1)
    while spare > 0:
        free = [i for i in range(1, amount) if given[i] < largest] or [i for i in range(1, amount) if given[i] < reach]
        pool, left = sum([portions[i] for i in free]), spare
        for i in free:
            addition = min(reach - given[i], max(1, left * portions[i] // pool), spare)
            given[i] = given[i] + addition
            spare = spare - addition
    return np.array(given)


def normal_values(stream_key, dims, width, most, cuts=(), kind=jnp.bfloat16):
    entries = jax.random.normal(stream_key, dims, jnp.float32) * width
    if len(cuts) > 0:
        entries = block_levels(stream_key, dims, cuts, -0.22, 0.18) * entries
    return jnp.clip(entries, min=-most, max=most).astype(kind)


def setup_inputs(seed: int = 0) -> dict:
    arg_keys = jax.random.split(jax.random.key(seed), 21)
    layer_in = normal_values(arg_keys[0], (SEQS, D), 1.0, 6.0, ((0, 16),))
    attn_gain = jnp.clip(1.0 + 0.18 * jax.random.normal(arg_keys[1], (D,), jnp.float32), 0.1, 1.9)
    query_weight = normal_values(arg_keys[2], (D, HEADS * HD), D ** -0.5, 0.125, ((1, 16),))
    key_weight = normal_values(arg_keys[3], (D, HEADS * HD), D ** -0.5, 0.125, ((1, 16),))
    value_weight = normal_values(arg_keys[4], (D, HEADS * HD), D ** -0.5, 0.125, ((1, 16),))
    forget_weight = normal_values(arg_keys[5], (D, HEADS), D ** -0.5, 0.125)
    forget_bias = jnp.clip(jax.random.uniform(arg_keys[6], (HEADS,), jnp.float32, -2.0, 3.0), -2.0, 3.0)
    out_weight = normal_values(arg_keys[7], (HEADS * HD, D), (HEADS * HD) ** -0.5, 0.1875, ((0, 16),))
    kv_cache = draw_kv_cache(jax.random.fold_in(arg_keys[20], 71), 0)
    cum_gates = draw_cum_gates(jax.random.fold_in(arg_keys[20], 71), 0)
    lengths = draw_lengths(jax.random.fold_in(arg_keys[20], 71), 0)
    ffn_gain = jnp.clip(1.0 + 0.18 * jax.random.normal(arg_keys[11], (D,), jnp.float32), 0.1, 1.9)
    route_ids_keys = jax.random.split(jax.random.fold_in(arg_keys[12], 1), SEQS // SEQ_GRP)
    route_ids_turns = jax.random.permutation(jax.random.fold_in(arg_keys[12], 3), SEQS // SEQ_GRP)
    route_ids = jax.vmap(lambda own, number: deal_out(jax.random.fold_in(arg_keys[12], 2), own, number, SEQ_GRP, EXPERTS, TOPK, CAP, 2))(route_ids_keys, route_ids_turns).reshape((SEQS, TOPK))
    route_weights = jnp.clip(jnp.exp(math.log(1.0) - 2.3025851 * jax.random.uniform(arg_keys[13], (SEQS, TOPK), jnp.float32) ** block_levels(arg_keys[13], (SEQS, TOPK), ((0, 16),), -0.2, 0.2)), 0.1, 1.0)
    shared_gate = normal_values(arg_keys[14], (D, SFF), D ** -0.5, 0.125, ((1, 16),))
    shared_up = normal_values(arg_keys[15], (D, SFF), D ** -0.5, 0.125, ((1, 16),))
    shared_down = normal_values(arg_keys[16], (SFF, D), SFF ** -0.5, 0.25, ((0, 16),))
    expert_gate = normal_values(arg_keys[17], (2 * EXPERTS, D, EFF // 2), D ** -0.5, 0.125, ((0, 256),))
    expert_up = normal_values(arg_keys[18], (2 * EXPERTS, D, EFF // 2), D ** -0.5, 0.125, ((0, 256),))
    expert_down = normal_values(arg_keys[19], (2 * EXPERTS, EFF // 2, D), EFF ** -0.5, 0.25, ((0, 256),))
    return dict(layer_in=layer_in, attn_gain=attn_gain, query_weight=query_weight, key_weight=key_weight, value_weight=value_weight, forget_weight=forget_weight, forget_bias=forget_bias, out_weight=out_weight, kv_cache=kv_cache, cum_gates=cum_gates, lengths=lengths, ffn_gain=ffn_gain, route_ids=route_ids, route_weights=route_weights, shared_gate=shared_gate, shared_up=shared_up, shared_down=shared_down, expert_gate=expert_gate, expert_up=expert_up, expert_down=expert_down)


NORM_EPS = 1e-06

def rms_scale(stream, gain):
    wide = stream.astype(jnp.float32)
    factor = lax.rsqrt(lax.optimization_barrier(jnp.mean(wide * wide, axis=-1, keepdims=True)) + NORM_EPS)
    return (wide * factor * gain.astype(jnp.float32)).astype(jnp.bfloat16)

def attend(queries, new_key, new_value, forget, kv_block, cum_block, length_block):
    head_size = queries.shape[-1]
    cache_span = kv_block.shape[2]
    positions = jnp.arange(cache_span, dtype=jnp.int32)
    inside = positions[None, None, :] < length_block[:, None, None]
    at_last = positions[None, None, :] == (length_block - 1)[:, None, None]
    latest = lax.optimization_barrier(jnp.sum(jnp.where(at_last, cum_block, 0.0), axis=-1))
    scaling = head_size ** (-0.5)
    cached_keys = kv_block[..., :head_size].astype(jnp.float32)
    cached_values = kv_block[..., head_size:].astype(jnp.float32)
    scores = jnp.einsum('shd,shld->shl', queries.astype(jnp.float32), cached_keys) * scaling
    scores = jnp.where(inside, scores + (latest + forget)[..., None] - cum_block, -jnp.inf)
    itself = lax.optimization_barrier(jnp.sum(queries.astype(jnp.float32) * new_key.astype(jnp.float32), axis=-1)) * scaling
    highest = jnp.maximum(lax.optimization_barrier(jnp.max(scores, axis=-1)), itself)
    earlier = jnp.exp(scores - highest[..., None])
    own_term = jnp.exp(itself - highest)
    denominator = lax.optimization_barrier(jnp.sum(earlier, axis=-1)) + own_term
    past_probs = (earlier / denominator[..., None]).astype(jnp.bfloat16)
    own_probs = (own_term / denominator).astype(jnp.bfloat16)
    blended = jnp.einsum('shl,shld->shd', past_probs.astype(jnp.float32), cached_values)
    blended = blended + own_probs.astype(jnp.float32)[..., None] * new_value.astype(jnp.float32)
    return blended.astype(jnp.bfloat16)

def reference(layer_in, attn_gain, query_weight, key_weight, value_weight, forget_weight, forget_bias, out_weight, kv_cache, cum_gates, lengths, ffn_gain, route_ids, route_weights, shared_gate, shared_up, shared_down, expert_gate, expert_up, expert_down):
    normed = rms_scale(layer_in, attn_gain)
    queries = jnp.dot(normed, query_weight, preferred_element_type=jnp.float32).astype(jnp.bfloat16).reshape(SEQS, HEADS, HD)
    new_key = jnp.dot(normed, key_weight, preferred_element_type=jnp.float32).astype(jnp.bfloat16).reshape(SEQS, HEADS, HD)
    new_value = jnp.dot(normed, value_weight, preferred_element_type=jnp.float32).astype(jnp.bfloat16).reshape(SEQS, HEADS, HD)
    new_kv = jnp.concatenate([new_key, new_value], axis=-1)
    forget = jax.nn.log_sigmoid(jnp.dot(normed, forget_weight, preferred_element_type=jnp.float32) + forget_bias)

    def group_attend(pieces):
        return attend(*pieces)
    attended = lax.map(group_attend, (queries.reshape(N_EP, SEQ_GRP, HEADS, HD), new_key.reshape(N_EP, SEQ_GRP, HEADS, HD), new_value.reshape(N_EP, SEQ_GRP, HEADS, HD), forget.reshape(N_EP, SEQ_GRP, HEADS), kv_cache.reshape(N_EP, SEQ_GRP, HEADS, CACHE_LENGTH, 2 * HD), cum_gates.reshape(N_EP, SEQ_GRP, HEADS, CACHE_LENGTH), lengths.reshape(N_EP, SEQ_GRP)))
    attended = attended.reshape(SEQS, HEADS * HD)
    head_out = jnp.dot(attended, out_weight, preferred_element_type=jnp.float32)
    middle = (layer_in.astype(jnp.float32) + head_out).astype(jnp.bfloat16)
    hidden_in = rms_scale(middle, ffn_gain)
    shared_hidden = (jax.nn.silu(jnp.dot(hidden_in, shared_gate, preferred_element_type=jnp.float32)) * jnp.dot(hidden_in, shared_up, preferred_element_type=jnp.float32)).astype(jnp.bfloat16)
    shared_out = jnp.dot(shared_hidden, shared_down, preferred_element_type=jnp.float32)
    expert_numbers = jnp.arange(EXPERTS, dtype=jnp.int32)
    combine = lax.optimization_barrier(jnp.sum(jnp.where(route_ids[:, :, None] == expert_numbers[None, None, :], route_weights[:, :, None], 0.0), axis=1))
    slot_count = N_EP * CAP
    gate_halves = expert_gate.reshape(EXPERTS, 2, D, EFF // 2)
    up_halves = expert_up.reshape(EXPERTS, 2, D, EFF // 2)
    down_halves = expert_down.reshape(EXPERTS, 2, EFF // 2, D)

    def one_expert(running, pieces):
        gate_half, up_half, down_half, column = pieces
        chosen = column > 0.0
        picked = jnp.nonzero(chosen, size=slot_count, fill_value=0)[0].astype(jnp.int32)
        filled = jnp.arange(slot_count, dtype=jnp.int32) < jnp.sum(chosen.astype(jnp.int32))
        batch_rows = hidden_in[picked]
        gate_full = jnp.concatenate([gate_half[0], gate_half[1]], axis=1)
        up_full = jnp.concatenate([up_half[0], up_half[1]], axis=1)
        down_full = jnp.concatenate([down_half[0], down_half[1]], axis=0)
        hidden = (jax.nn.silu(jnp.dot(batch_rows, gate_full, preferred_element_type=jnp.float32)) * jnp.dot(batch_rows, up_full, preferred_element_type=jnp.float32)).astype(jnp.bfloat16)
        result = jnp.dot(hidden, down_full, preferred_element_type=jnp.float32)
        shares = jnp.where(filled, column[picked], 0.0)
        return (running.at[picked].add(shares[:, None] * result), None)
    routed, _ = lax.scan(one_expert, jnp.zeros((SEQS, D), jnp.float32), (gate_halves, up_halves, down_halves, combine.T))
    layer_out = (middle.astype(jnp.float32) + shared_out + routed).astype(jnp.bfloat16)
    return (layer_out, new_kv)
```

```python
import jax
import jax.numpy as jnp
from jax import lax
from jax.experimental import pallas as pl
from jax.experimental.pallas import tpu as pltpu
from jax.sharding import PartitionSpec as P

NORM_EPS = 1e-06
MESH = pl.DeviceIdType.MESH
BF = jnp.bfloat16
F32 = jnp.float32
N = 16
ROWS = 32
WIDTH = 2048
LANES = 128
SPAN = 1024
HEAD = 64
TP_ORDER = (8, 9, 7, 6, 10, 11, 5, 4, 12, 13, 3, 2, 14, 15, 1)
EP_ORDER = (10, 6, 14, 9, 11, 2, 8, 5, 7, 13, 15, 1, 3, 4, 12)
KV_COPIES = 16


def nn(a, b):
    return jnp.dot(a, b, preferred_element_type=F32)


def nt(a, b):
    return lax.dot_general(a, b, (((1,), (1,)), ((), ())), preferred_element_type=F32)


def silu(v):
    return v / (1.0 + jnp.exp(-v))


def layer_kernel(
    x_h, ag_h, wq_h, wk_h, wv_h, wf_h, fb_h, wo_h, kv_h, cum_h, len_h, fg_h,
    ids_h, rw_h, sg_h, su_h, sd_h, eg_h, eu_h, ed_h,
    out_ref, nkv_ref,
    x_v, ag_v, w_v, fb_v, wo_v, kv_v, cum_v, len_v, fg_v,
    ids_v, rw_v, sg_v, su_v, sd_v, eg_v, eu_v, ed_v,
    part_s, part_r, mid_a, dsp_s, dsp_r, ret_s, ret_r, fin_s, fin_r, out_a, shared_v,
    lsem, ksem, send_sem, recv_sem,
):
    ep = lax.axis_index("ep")
    tp = lax.axis_index("tp")

    copies = [
        (x_h, x_v), (ag_h, ag_v),
        (wk_h, w_v.at[pl.ds(0, HEAD)]), (wv_h, w_v.at[pl.ds(HEAD, HEAD)]),
        (wq_h, w_v.at[pl.ds(2 * HEAD, HEAD)]), (wf_h, w_v.at[pl.ds(3 * HEAD, N)]),
        (fb_h, fb_v), (cum_h, cum_v), (len_h, len_v),
        (wo_h, wo_v.at[pl.ds(HEAD, HEAD)]), (ids_h, ids_v), (rw_h, rw_v), (fg_h, fg_v),
        (sg_h, sg_v), (su_h, su_v), (sd_h, sd_v), (eg_h, eg_v), (eu_h, eu_v), (ed_h, ed_v),
    ]
    local = [pltpu.make_async_copy(s, d, lsem.at[i]) for i, (s, d) in enumerate(copies)]
    per = ROWS // KV_COPIES
    cached = [
        pltpu.make_async_copy(kv_h.at[pl.ds(i * per, per)], kv_v.at[pl.ds(i * per, per)], ksem.at[i])
        for i in range(KV_COPIES)
    ]
    for c in local[:9]:
        c.start()
    for c in cached:
        c.start()
    for c in local[9:]:
        c.start()

    barrier = pltpu.get_barrier_semaphore()
    for j in range(1, N):
        pl.semaphore_signal(barrier, inc=1, device_id=(ep, lax.rem(tp + j, N)), device_id_type=MESH)
        pl.semaphore_signal(barrier, inc=1, device_id=(lax.rem(ep + j, N), tp), device_id_type=MESH)

    def all_sent(phase, ref):
        pltpu.make_async_remote_copy(
            src_ref=ref, dst_ref=ref, send_sem=send_sem.at[phase], recv_sem=recv_sem.at[phase],
            device_id=(ep, lax.rem(tp + 1, N)), device_id_type=MESH,
        ).wait_send()

    def all_arrived(phase, ref):
        pltpu.make_async_remote_copy(
            src_ref=ref, dst_ref=ref, send_sem=send_sem.at[phase], recv_sem=recv_sem.at[phase],
            device_id=(ep, lax.rem(tp + 1, N)), device_id_type=MESH,
        ).wait_recv()

    def push(phase, src, dst, device):
        pltpu.make_async_remote_copy(
            src_ref=src, dst_ref=dst, send_sem=send_sem.at[phase], recv_sem=recv_sem.at[phase],
            device_id=device, device_id_type=MESH,
        ).start()

    def scatter_tp(phase, src, dst):
        for j in TP_ORDER:
            to = lax.rem(tp + j, N)
            push(phase, src.at[to], dst.at[j - 1], (ep, to))

    def gather_tp(phase, ref):
        for j in TP_ORDER:
            push(phase, ref.at[tp], ref.at[tp], (ep, lax.rem(tp + j, N)))

    def exchange_ep(phase, src, dst):
        for i in EP_ORDER:
            to = lax.rem(ep + i, N)
            push(phase, src.at[:, to], dst.at[:, ep], (to, tp))

    w_v[pl.ds(3 * HEAD + N, HEAD - N)] = jnp.zeros((HEAD - N, WIDTH), BF)
    wo_v[pl.ds(0, HEAD)] = jnp.zeros((HEAD, WIDTH), BF)

    for c in local[:7]:
        c.wait()
    wide = x_v[...].astype(F32)
    factor = lax.rsqrt(jnp.mean(wide * wide, axis=-1, keepdims=True) + NORM_EPS)
    normed = (wide * factor * ag_v[...]).astype(BF)
    res = nt(normed, w_v[...])
    nkv = res[:, :LANES].astype(BF)
    nkv_ref[...] = nkv
    nkv_f = nkv.astype(F32)
    rest = res[:, LANES:]
    lane = lax.broadcasted_iota(jnp.int32, (ROWS, LANES), 1)
    q_f = jnp.where(lane < HEAD, rest, 0.0).astype(BF).astype(F32)
    bias = jnp.sum(
        jnp.where(lax.broadcasted_iota(jnp.int32, (1, N), 1) == tp, fb_v[...], 0.0),
        axis=-1, keepdims=True,
    )
    logit = jnp.sum(jnp.where(lane == HEAD + tp, rest, 0.0), axis=-1, keepdims=True) + bias
    forget = jnp.minimum(logit, 0.0) - jnp.log(1.0 + jnp.exp(-jnp.abs(logit)))
    scaling = HEAD ** (-0.5)
    itself = jnp.sum(q_f * nkv_f, axis=-1, keepdims=True) * scaling

    local[7].wait()
    local[8].wait()
    diag = lax.broadcasted_iota(jnp.int32, (ROWS, ROWS), 0) == lax.broadcasted_iota(
        jnp.int32, (ROWS, ROWS), 1
    )
    length = jnp.sum(
        jnp.where(diag, len_v[...].astype(F32), 0.0), axis=-1, keepdims=True
    ).astype(jnp.int32)
    position = lax.broadcasted_iota(jnp.int32, (8, SPAN), 1)
    row8 = lax.broadcasted_iota(jnp.int32, (8, LANES), 0)
    pieces = []
    for g in range(ROWS // 8):
        here = slice(8 * g, 8 * g + 8)
        for c in cached[8 // per * g : 8 // per * (g + 1)]:
            c.wait()
        q8 = q_f[here]
        scores = jnp.zeros((8, SPAN), F32)
        for p in range(4):
            asked = jnp.concatenate(
                [jnp.where(row8 == 2 * p, q8, 0.0), jnp.where(row8 == 2 * p + 1, q8, 0.0)], axis=1
            ).astype(BF)
            pair = jnp.concatenate([kv_v[8 * g + 2 * p], kv_v[8 * g + 2 * p + 1]], axis=1)
            scores = scores + nt(asked, pair)
        cum = cum_v[pl.ds(8 * g, 8), 0, :]
        len8 = length[here]
        latest = jnp.sum(jnp.where(position == len8 - 1, cum, 0.0), axis=-1, keepdims=True)
        scores = scores * scaling + (latest + forget[here]) - cum
        scores = jnp.where(position < len8, scores, -jnp.inf)
        highest = jnp.maximum(jnp.max(scores, axis=-1, keepdims=True), itself[here])
        earlier = jnp.exp(scores - highest)
        own = jnp.exp(itself[here] - highest)
        denominator = jnp.sum(earlier, axis=-1, keepdims=True) + own
        probs = (earlier / denominator).astype(BF)
        att = (own / denominator).astype(BF).astype(F32) * nkv_f[here]
        for p in range(4):
            pair = jnp.concatenate([kv_v[8 * g + 2 * p], kv_v[8 * g + 2 * p + 1]], axis=1)
            o = nn(probs, pair)
            att = att + jnp.where(row8 == 2 * p, o[:, :LANES], 0.0)
            att = att + jnp.where(row8 == 2 * p + 1, o[:, LANES:], 0.0)
        pieces.append(att)
    attended = jnp.where(lane >= HEAD, jnp.concatenate(pieces, axis=0), 0.0).astype(BF)

    local[9].wait()
    head_part = nn(attended, wo_v[...]).astype(BF)
    for c in range(N):
        part_s[c] = head_part[:, c * LANES : (c + 1) * LANES]
    pl.semaphore_wait(barrier, 2 * (N - 1))
    scatter_tp(0, part_s, part_r)

    for c in local[10:13]:
        c.wait()
    slot = lax.broadcasted_iota(jnp.int32, (ROWS, ROWS), 0)
    target = (slot // 2) * (N // 2) + tp // 2
    member = jnp.zeros((ROWS, ROWS), F32)
    weight = jnp.zeros((ROWS, ROWS), F32)
    for k in range(ids_v.shape[0]):
        hit = ids_v[pl.ds(k, 1), :] == target
        member = jnp.where(hit, 1.0, member)
        weight = weight + jnp.where(hit, rw_v[pl.ds(k, 1), :], 0.0)
    before = (slot < lax.broadcasted_iota(jnp.int32, (ROWS, ROWS), 1)).astype(F32).astype(BF)
    rank = nn(member.astype(BF), before)
    placed = (member > 0.5) & (jnp.abs(rank - (slot % 2).astype(F32)) < 0.5)
    placement = jnp.where(placed, 1.0, 0.0).astype(BF)
    shares = jnp.where(placed, weight, 0.0)
    high = shares.astype(BF)
    low = (shares - high.astype(F32)).astype(BF)
    unit = jnp.where(diag, 1.0, 0.0).astype(BF)
    high = nt(unit, high).astype(BF)
    low = nt(unit, low).astype(BF)

    all_arrived(0, part_r)
    total = part_s[tp].astype(F32)
    for j in range(N - 1):
        total = total + part_r[j].astype(F32)
    own_stream = x_v[:, pl.ds(pl.multiple_of(tp * LANES, LANES), LANES)].astype(F32)
    mid_a[tp] = (own_stream + total).astype(BF)
    gather_tp(1, mid_a)
    all_arrived(1, mid_a.at[pl.ds(0, N - 1)])

    square = jnp.zeros((ROWS, LANES), F32)
    for c in range(N):
        m = mid_a[c].astype(F32)
        square = square + m * m
    factor = lax.rsqrt(jnp.sum(square, axis=-1, keepdims=True) * (1.0 / WIDTH) + NORM_EPS)
    hidden_in = jnp.concatenate(
        [
            (mid_a[c].astype(F32) * factor * fg_v[:, c * LANES : (c + 1) * LANES]).astype(BF)
            for c in range(N)
        ],
        axis=1,
    )
    dispatch = nn(placement, hidden_in).astype(BF)
    dsp_rows = dsp_s.reshape(N, ROWS, LANES)
    for c in range(N):
        dsp_rows[c] = dispatch[:, c * LANES : (c + 1) * LANES]
    exchange_ep(2, dsp_s, dsp_r)

    for c in local[13:16]:
        c.wait()
    shared_hidden = (silu(nt(hidden_in, sg_v[...])) * nt(hidden_in, su_v[...])).astype(BF)
    shared_v[...] = nn(shared_hidden, sd_v[...])
    for c in local[16:]:
        c.wait()

    mine = lax.broadcasted_iota(jnp.int32, (ROWS, LANES), 0) // 2 == ep

    def merged(kept, came):
        kept, came = kept.reshape(N, ROWS, LANES), came.reshape(N, ROWS, LANES)
        return jnp.concatenate(
            [
                jnp.where(mine, kept[c].astype(F32), came[c].astype(F32)).astype(BF)
                for c in range(N)
            ],
            axis=1,
        )

    all_arrived(2, dsp_r.at[pl.ds(0, N - 1)])
    batch = merged(dsp_s, dsp_r)
    hidden = (silu(nn(batch, eg_v[...])) * nn(batch, eu_v[...])).astype(BF)
    served = nn(hidden, ed_v[...]).astype(BF)
    ret_rows = ret_s.reshape(N, ROWS, LANES)
    for c in range(N):
        ret_rows[c] = served[:, c * LANES : (c + 1) * LANES]
    exchange_ep(3, ret_s, ret_r)
    all_arrived(3, ret_r.at[pl.ds(0, N - 1)])

    returned = merged(ret_s, ret_r)
    mixed = (shared_v[...] + (nn(high, returned) + nn(low, returned))).astype(BF)
    for c in range(N):
        fin_s[c] = mixed[:, c * LANES : (c + 1) * LANES]
    scatter_tp(4, fin_s, fin_r)
    all_arrived(4, fin_r)
    total = mid_a[tp].astype(F32) + fin_s[tp].astype(F32)
    for j in range(N - 1):
        total = total + fin_r[j].astype(F32)
    out_a[tp] = total.astype(BF)
    gather_tp(5, out_a)
    all_arrived(5, out_a.at[pl.ds(0, N - 1)])
    for c in range(N):
        out_ref[:, c * LANES : (c + 1) * LANES] = out_a[c]

    for phase in range(6):
        all_sent(phase, part_r)


def body(
    layer_in, attn_gain, query_weight, key_weight, value_weight, forget_weight, forget_bias,
    out_weight, kv_cache, cum_gates, lengths, ffn_gain, route_ids, route_weights,
    shared_gate, shared_up, shared_down, expert_gate, expert_up, expert_down,
):
    operands = (
        layer_in, attn_gain.reshape(1, -1), query_weight.T, key_weight.T, value_weight.T,
        forget_weight.T, forget_bias.reshape(1, -1), out_weight, kv_cache[:, 0], cum_gates,
        lengths.reshape(1, -1), ffn_gain.reshape(1, -1), route_ids.T, route_weights.T,
        shared_gate.T, shared_up.T, shared_down, expert_gate[0], expert_up[0], expert_down[0],
    )
    picks = route_ids.shape[1]
    block = (N, ROWS, LANES)
    paired = (N, N, 2, LANES)
    layer_out, new_kv = pl.pallas_call(
        layer_kernel,
        out_shape=(
            jax.ShapeDtypeStruct((ROWS, WIDTH), BF),
            jax.ShapeDtypeStruct((ROWS, LANES), BF),
        ),
        in_specs=[pl.BlockSpec(memory_space=pltpu.HBM)] * len(operands),
        out_specs=[pl.BlockSpec(memory_space=pltpu.VMEM)] * 2,
        scratch_shapes=[
            pltpu.VMEM((ROWS, WIDTH), BF),
            pltpu.VMEM((1, WIDTH), F32),
            pltpu.VMEM((4 * HEAD, WIDTH), BF),
            pltpu.VMEM((1, N), F32),
            pltpu.VMEM((2 * HEAD, WIDTH), BF),
            pltpu.VMEM((ROWS, SPAN, LANES), BF),
            pltpu.VMEM((ROWS, 1, SPAN), F32),
            pltpu.VMEM((1, ROWS), jnp.int32),
            pltpu.VMEM((1, WIDTH), F32),
            pltpu.VMEM((picks, ROWS), jnp.int32),
            pltpu.VMEM((picks, ROWS), F32),
            pltpu.VMEM((ROWS, WIDTH), BF),
            pltpu.VMEM((ROWS, WIDTH), BF),
            pltpu.VMEM((ROWS, WIDTH), BF),
            pltpu.VMEM((WIDTH, 4 * HEAD), BF),
            pltpu.VMEM((WIDTH, 4 * HEAD), BF),
            pltpu.VMEM((4 * HEAD, WIDTH), BF),
            pltpu.VMEM(block, BF),
            pltpu.VMEM((N - 1, ROWS, LANES), BF),
            pltpu.VMEM(block, BF),
            pltpu.VMEM(paired, BF),
            pltpu.VMEM(paired, BF),
            pltpu.VMEM(paired, BF),
            pltpu.VMEM(paired, BF),
            pltpu.VMEM(block, BF),
            pltpu.VMEM((N - 1, ROWS, LANES), BF),
            pltpu.VMEM(block, BF),
            pltpu.VMEM((ROWS, WIDTH), F32),
            pltpu.SemaphoreType.DMA((len(operands) - 1,)),
            pltpu.SemaphoreType.DMA((KV_COPIES,)),
            pltpu.SemaphoreType.DMA((6,)),
            pltpu.SemaphoreType.DMA((6,)),
        ],
        compiler_params=pltpu.CompilerParams(collective_id=0, has_side_effects=True),
        name="decode_layer",
    )(*operands)
    return (layer_out, new_kv[:, None, :])


def solution(mesh):
    placed = (
        P("ep", None), P(), P(None, "tp"), P(None, "tp"), P(None, "tp"), P(), P(), P("tp", None),
        P("ep", "tp", None, None), P("ep", "tp", None), P("ep"), P(), P("ep", None),
        P("ep", None), P(None, "tp"), P(None, "tp"), P("tp", None), P(("ep", "tp"), None, None),
        P(("ep", "tp"), None, None), P(("ep", "tp"), None, None),
    )
    return jax.shard_map(
        body,
        mesh=mesh,
        in_specs=placed,
        out_specs=(P("ep", None), P("ep", "tp", None)),
        check_vma=False,
    )
```

```python
import jax
import jax.numpy as jnp
from jax import lax
from jax.experimental import pallas as pl
from jax.experimental.pallas import tpu as pltpu
from jax.sharding import PartitionSpec as P

NORM_EPS = 1e-06
MESH = pl.DeviceIdType.MESH
BF = jnp.bfloat16
F32 = jnp.float32
N = 16
ROWS = 32
WIDTH = 2048
LANES = 128
SPAN = 1024
HEAD = 64
TP_ORDER = (8, 9, 7, 6, 10, 11, 5, 4, 12, 13, 3, 2, 14, 15, 1)
KV_COPIES = 16


def nn(a, b):
    return jnp.dot(a, b, preferred_element_type=F32)


def nt(a, b):
    return lax.dot_general(a, b, (((1,), (1,)), ((), ())), preferred_element_type=F32)


def silu(v):
    return v / (1.0 + jnp.exp(-v))


def layer_kernel(
    x_h, ag_h, wq_h, wk_h, wv_h, wf_h, fb_h, wo_h, kv_h, cum_h, len_h, fg_h,
    ids_h, rw_h, sg_h, su_h, sd_h, eg_h, eu_h, ed_h,
    out_ref, nkv_ref,
    x_v, ag_v, w_v, fb_v, wo_v, kv_v, cum_v, len_v, fg_v,
    ids_v, rw_v, sg_v, su_v, sd_v, eg_v, eu_v, ed_v,
    part_s, part_r, mid_a, dsp_s, dsp_r, ret_s, ret_r, fin_s, fin_r, out_a,
    lsem, ksem, send_sem, recv_sem, ready,
):
    ep = lax.axis_index("ep")
    tp = lax.axis_index("tp")

    copies = [
        (x_h, x_v), (ag_h, ag_v),
        (wk_h, w_v.at[pl.ds(0, HEAD)]), (wv_h, w_v.at[pl.ds(HEAD, HEAD)]),
        (wq_h, w_v.at[pl.ds(2 * HEAD, HEAD)]), (wf_h, w_v.at[pl.ds(3 * HEAD, N)]),
        (fb_h, fb_v), (cum_h, cum_v), (len_h, len_v),
        (wo_h, wo_v.at[pl.ds(HEAD, HEAD)]), (ids_h, ids_v), (rw_h, rw_v), (fg_h, fg_v),
        (sg_h, sg_v), (su_h, su_v), (sd_h, sd_v), (eg_h, eg_v), (eu_h, eu_v), (ed_h, ed_v),
    ]
    local = [pltpu.make_async_copy(s, d, lsem.at[i]) for i, (s, d) in enumerate(copies)]
    per = ROWS // KV_COPIES
    cached = [
        pltpu.make_async_copy(kv_h.at[pl.ds(i * per, per)], kv_v.at[pl.ds(i * per, per)], ksem.at[i])
        for i in range(KV_COPIES)
    ]
    for c in local[:9]:
        c.start()
    for c in cached:
        c.start()
    for c in local[9:]:
        c.start()

    barrier = pltpu.get_barrier_semaphore()
    for j in range(1, N):
        pl.semaphore_signal(barrier, inc=1, device_id=(ep, lax.rem(tp + j, N)), device_id_type=MESH)
        pl.semaphore_signal(barrier, inc=1, device_id=(lax.rem(ep + j, N), tp), device_id_type=MESH)

    def all_sent(phase, ref):
        pltpu.make_async_remote_copy(
            src_ref=ref, dst_ref=ref, send_sem=send_sem.at[phase], recv_sem=recv_sem.at[phase],
            device_id=(ep, lax.rem(tp + 1, N)), device_id_type=MESH,
        ).wait_send()

    def all_arrived(phase, ref):
        pltpu.make_async_remote_copy(
            src_ref=ref, dst_ref=ref, send_sem=send_sem.at[phase], recv_sem=recv_sem.at[phase],
            device_id=(ep, lax.rem(tp + 1, N)), device_id_type=MESH,
        ).wait_recv()

    def push(phase, src, dst, device):
        pltpu.make_async_remote_copy(
            src_ref=src, dst_ref=dst, send_sem=send_sem.at[phase], recv_sem=recv_sem.at[phase],
            device_id=device, device_id_type=MESH,
        ).start()

    def scatter_tp(phase, src, dst):
        for j in TP_ORDER:
            to = lax.rem(tp + j, N)
            push(phase, src.at[to], dst.at[j - 1], (ep, to))

    def gather_tp(phase, ref):
        for j in TP_ORDER:
            push(phase, ref.at[tp], ref.at[tp], (ep, lax.rem(tp + j, N)))

    def everywhere(phase, pick, dst):
        def to_ep(i, carry):
            far = lax.rem(ep + i, N)
            for j in (0,) + TP_ORDER:
                to = lax.rem(tp + j, N)
                push(phase, pick(far, to), dst, (far, to))
            return carry

        lax.fori_loop(1, N, to_ep, 0)
        for j in TP_ORDER:
            to = lax.rem(tp + j, N)
            push(phase, pick(ep, to), dst, (ep, to))

    w_v[pl.ds(3 * HEAD + N, HEAD - N)] = jnp.zeros((HEAD - N, WIDTH), BF)
    wo_v[pl.ds(0, HEAD)] = jnp.zeros((HEAD, WIDTH), BF)

    for c in local[:7]:
        c.wait()
    wide = x_v[...].astype(F32)
    factor = lax.rsqrt(jnp.mean(wide * wide, axis=-1, keepdims=True) + NORM_EPS)
    normed = (wide * factor * ag_v[...]).astype(BF)
    res = nt(normed, w_v[...])
    nkv = res[:, :LANES].astype(BF)
    nkv_ref[...] = nkv
    nkv_f = nkv.astype(F32)
    rest = res[:, LANES:]
    lane = lax.broadcasted_iota(jnp.int32, (ROWS, LANES), 1)
    q_f = jnp.where(lane < HEAD, rest, 0.0).astype(BF).astype(F32)
    bias = jnp.sum(
        jnp.where(lax.broadcasted_iota(jnp.int32, (1, N), 1) == tp, fb_v[...], 0.0),
        axis=-1, keepdims=True,
    )
    logit = jnp.sum(jnp.where(lane == HEAD + tp, rest, 0.0), axis=-1, keepdims=True) + bias
    forget = jnp.minimum(logit, 0.0) - jnp.log(1.0 + jnp.exp(-jnp.abs(logit)))
    scaling = HEAD ** (-0.5)
    itself = jnp.sum(q_f * nkv_f, axis=-1, keepdims=True) * scaling

    local[7].wait()
    local[8].wait()
    diag = lax.broadcasted_iota(jnp.int32, (ROWS, ROWS), 0) == lax.broadcasted_iota(
        jnp.int32, (ROWS, ROWS), 1
    )
    length = jnp.sum(
        jnp.where(diag, len_v[...].astype(F32), 0.0), axis=-1, keepdims=True
    ).astype(jnp.int32)
    position = lax.broadcasted_iota(jnp.int32, (8, SPAN), 1)
    row8 = lax.broadcasted_iota(jnp.int32, (8, LANES), 0)
    pieces = []
    for g in range(ROWS // 8):
        here = slice(8 * g, 8 * g + 8)
        for c in cached[8 // per * g : 8 // per * (g + 1)]:
            c.wait()
        q8 = q_f[here]
        scores = jnp.zeros((8, SPAN), F32)
        for p in range(4):
            asked = jnp.concatenate(
                [jnp.where(row8 == 2 * p, q8, 0.0), jnp.where(row8 == 2 * p + 1, q8, 0.0)], axis=1
            ).astype(BF)
            pair = jnp.concatenate([kv_v[8 * g + 2 * p], kv_v[8 * g + 2 * p + 1]], axis=1)
            scores = scores + nt(asked, pair)
        cum = cum_v[pl.ds(8 * g, 8), 0, :]
        len8 = length[here]
        latest = jnp.sum(jnp.where(position == len8 - 1, cum, 0.0), axis=-1, keepdims=True)
        scores = scores * scaling + (latest + forget[here]) - cum
        scores = jnp.where(position < len8, scores, -jnp.inf)
        highest = jnp.maximum(jnp.max(scores, axis=-1, keepdims=True), itself[here])
        earlier = jnp.exp(scores - highest)
        own = jnp.exp(itself[here] - highest)
        denominator = jnp.sum(earlier, axis=-1, keepdims=True) + own
        probs = (earlier / denominator).astype(BF)
        att = (own / denominator).astype(BF).astype(F32) * nkv_f[here]
        for p in range(4):
            pair = jnp.concatenate([kv_v[8 * g + 2 * p], kv_v[8 * g + 2 * p + 1]], axis=1)
            o = nn(probs, pair)
            att = att + jnp.where(row8 == 2 * p, o[:, :LANES], 0.0)
            att = att + jnp.where(row8 == 2 * p + 1, o[:, LANES:], 0.0)
        pieces.append(att)
    attended = jnp.where(lane >= HEAD, jnp.concatenate(pieces, axis=0), 0.0).astype(BF)

    local[9].wait()
    head_part = nn(attended, wo_v[...]).astype(BF)
    for c in range(N):
        part_s[c] = head_part[:, c * LANES : (c + 1) * LANES]
    pl.semaphore_wait(barrier, 2 * (N - 1))
    for j in range(1, N):
        pl.semaphore_signal(
            ready, inc=1, device_id=(lax.rem(ep + j, N), tp), device_id_type=MESH
        )
    scatter_tp(0, part_s, part_r)

    for c in local[10:13]:
        c.wait()
    experts = N * N // 2
    slot = lax.broadcasted_iota(jnp.int32, (2 * experts, ROWS), 0)
    target = slot // 2
    member = jnp.zeros(slot.shape, F32)
    weight = jnp.zeros(slot.shape, F32)
    for k in range(ids_v.shape[0]):
        hit = ids_v[pl.ds(k, 1), :] == target
        member = jnp.where(hit, 1.0, member)
        weight = weight + jnp.where(hit, rw_v[pl.ds(k, 1), :], 0.0)
    before = jnp.where(
        lax.broadcasted_iota(jnp.int32, (ROWS, ROWS), 0)
        < lax.broadcasted_iota(jnp.int32, (ROWS, ROWS), 1),
        1.0,
        0.0,
    ).astype(BF)
    rank = nn(member.astype(BF), before)
    placed = (member > 0.5) & (jnp.abs(rank - (slot % 2).astype(F32)) < 0.5)
    placement = jnp.where(placed, 1.0, 0.0).astype(BF)
    shares = jnp.where(placed, weight, 0.0)
    high = shares.astype(BF)
    low = (shares - high.astype(F32)).astype(BF)
    unit = jnp.where(diag, 1.0, 0.0).astype(BF)
    high = nt(unit, high).astype(BF)
    low = nt(unit, low).astype(BF)

    all_arrived(0, part_r)
    total = part_s[tp].astype(F32)
    for j in range(N - 1):
        total = total + part_r[j].astype(F32)
    own_stream = x_v[:, pl.ds(pl.multiple_of(tp * LANES, LANES), LANES)].astype(F32)
    middle = (own_stream + total).astype(BF)
    mid_a[tp] = middle
    dsp_s.reshape(2 * experts, LANES)[...] = nn(placement, middle).astype(BF)
    pl.semaphore_wait(ready, N - 1)
    everywhere(2, lambda e, t: dsp_s.at[e * (N // 2) + t // 2], dsp_r.at[tp, ep])
    dsp_r[tp, ep] = dsp_s[ep * (N // 2) + tp // 2]
    gather_tp(1, mid_a)

    def normalised(blocks):
        square = jnp.zeros((ROWS, LANES), F32)
        for c in range(N):
            m = blocks[c].astype(F32)
            square = square + m * m
        factor = lax.rsqrt(jnp.sum(square, axis=-1, keepdims=True) * (1.0 / WIDTH) + NORM_EPS)
        return jnp.concatenate(
            [
                (blocks[c].astype(F32) * factor * fg_v[:, c * LANES : (c + 1) * LANES]).astype(BF)
                for c in range(N)
            ],
            axis=1,
        )

    for c in local[13:]:
        c.wait()
    all_arrived(2, dsp_r.reshape(N * N, 2, LANES).at[pl.ds(0, N * N - 1)])
    batch = normalised(dsp_r.reshape(N, ROWS, LANES))
    hidden = (silu(nn(batch, eg_v[...])) * nn(batch, eu_v[...])).astype(BF)
    served = nn(hidden, ed_v[...]).astype(BF)
    ret_rows = ret_s.reshape(N, ROWS, LANES)
    for c in range(N):
        ret_rows[c] = served[:, c * LANES : (c + 1) * LANES]
    mine = ep * (N // 2) + tp // 2
    everywhere(3, lambda e, t: ret_s.at[t, e], ret_r.at[lax.rem(tp, 2), mine])
    ret_r[lax.rem(tp, 2), mine] = ret_s[tp, ep]

    all_arrived(1, mid_a.at[pl.ds(0, N - 1)])
    hidden_in = normalised(mid_a)
    shared_hidden = (silu(nt(hidden_in, sg_v[...])) * nt(hidden_in, su_v[...])).astype(BF)
    mixed = nn(shared_hidden, sd_v[...]).astype(BF)
    for c in range(N):
        fin_s[c] = mixed[:, c * LANES : (c + 1) * LANES]
    scatter_tp(4, fin_s, fin_r)

    all_arrived(4, fin_r)
    total = mid_a[tp].astype(F32) + fin_s[tp].astype(F32)
    for j in range(N - 1):
        total = total + fin_r[j].astype(F32)
    all_arrived(3, ret_r.reshape(N * N, 2, LANES).at[pl.ds(0, N * N - 1)])
    ret_half = ret_r.reshape(2, 2 * experts, LANES)
    for c in range(2):
        returned = ret_half[c]
        total = total + nn(high, returned) + nn(low, returned)
    out_a[tp] = total.astype(BF)
    gather_tp(5, out_a)
    all_arrived(5, out_a.at[pl.ds(0, N - 1)])
    for c in range(N):
        out_ref[:, c * LANES : (c + 1) * LANES] = out_a[c]

    for phase in (0, 1, 4, 5):
        all_sent(phase, part_r)
    for phase in (2, 3):
        all_sent(phase, dsp_r.reshape(N * N, 2, LANES).at[pl.ds(0, N * N - 1)])


def body(
    layer_in, attn_gain, query_weight, key_weight, value_weight, forget_weight, forget_bias,
    out_weight, kv_cache, cum_gates, lengths, ffn_gain, route_ids, route_weights,
    shared_gate, shared_up, shared_down, expert_gate, expert_up, expert_down,
):
    operands = (
        layer_in, attn_gain.reshape(1, -1), query_weight.T, key_weight.T, value_weight.T,
        forget_weight.T, forget_bias.reshape(1, -1), out_weight, kv_cache[:, 0], cum_gates,
        lengths.reshape(1, -1), ffn_gain.reshape(1, -1), route_ids.T, route_weights.T,
        shared_gate.T, shared_up.T, shared_down, expert_gate[0], expert_up[0], expert_down[0],
    )
    picks = route_ids.shape[1]
    block = (N, ROWS, LANES)
    layer_out, new_kv = pl.pallas_call(
        layer_kernel,
        out_shape=(
            jax.ShapeDtypeStruct((ROWS, WIDTH), BF),
            jax.ShapeDtypeStruct((ROWS, LANES), BF),
        ),
        in_specs=[pl.BlockSpec(memory_space=pltpu.HBM)] * len(operands),
        out_specs=[pl.BlockSpec(memory_space=pltpu.VMEM)] * 2,
        scratch_shapes=[
            pltpu.VMEM((ROWS, WIDTH), BF),
            pltpu.VMEM((1, WIDTH), F32),
            pltpu.VMEM((4 * HEAD, WIDTH), BF),
            pltpu.VMEM((1, N), F32),
            pltpu.VMEM((2 * HEAD, WIDTH), BF),
            pltpu.VMEM((ROWS, SPAN, LANES), BF),
            pltpu.VMEM((ROWS, 1, SPAN), F32),
            pltpu.VMEM((1, ROWS), jnp.int32),
            pltpu.VMEM((1, WIDTH), F32),
            pltpu.VMEM((picks, ROWS), jnp.int32),
            pltpu.VMEM((picks, ROWS), F32),
            pltpu.VMEM((ROWS, WIDTH), BF),
            pltpu.VMEM((ROWS, WIDTH), BF),
            pltpu.VMEM((ROWS, WIDTH), BF),
            pltpu.VMEM((WIDTH, 4 * HEAD), BF),
            pltpu.VMEM((WIDTH, 4 * HEAD), BF),
            pltpu.VMEM((4 * HEAD, WIDTH), BF),
            pltpu.VMEM(block, BF),
            pltpu.VMEM((N - 1, ROWS, LANES), BF),
            pltpu.VMEM(block, BF),
            pltpu.VMEM((N * N // 2, 2, LANES), BF),
            pltpu.VMEM((N, N, 2, LANES), BF),
            pltpu.VMEM((N, N, 2, LANES), BF),
            pltpu.VMEM((2, N * N // 2, 2, LANES), BF),
            pltpu.VMEM(block, BF),
            pltpu.VMEM((N - 1, ROWS, LANES), BF),
            pltpu.VMEM(block, BF),
            pltpu.SemaphoreType.DMA((len(operands) - 1,)),
            pltpu.SemaphoreType.DMA((KV_COPIES,)),
            pltpu.SemaphoreType.DMA((6,)),
            pltpu.SemaphoreType.DMA((6,)),
            pltpu.SemaphoreType.REGULAR,
        ],
        compiler_params=pltpu.CompilerParams(collective_id=0, has_side_effects=True),
        name="decode_layer",
    )(*operands)
    return (layer_out, new_kv[:, None, :])


def solution(mesh):
    placed = (
        P("ep", None), P(), P(None, "tp"), P(None, "tp"), P(None, "tp"), P(), P(), P("tp", None),
        P("ep", "tp", None, None), P("ep", "tp", None), P("ep"), P(), P("ep", None),
        P("ep", None), P(None, "tp"), P(None, "tp"), P("tp", None), P(("ep", "tp"), None, None),
        P(("ep", "tp"), None, None), P(("ep", "tp"), None, None),
    )
    return jax.shard_map(
        body,
        mesh=mesh,
        in_specs=placed,
        out_specs=(P("ep", None), P("ep", "tp", None)),
        check_vma=False,
    )
```

```python
import jax
import jax.numpy as jnp
from jax import lax
from jax.experimental import pallas as pl
from jax.experimental.pallas import tpu as pltpu
from jax.sharding import PartitionSpec as P

NORM_EPS = 1e-06
MESH = pl.DeviceIdType.MESH
BF = jnp.bfloat16
F32 = jnp.float32
N = 16
ROWS = 32
WIDTH = 2048
LANES = 128
SPAN = 1024
HEAD = 64
TP_ORDER = (8, 9, 7, 6, 10, 11, 5, 4, 12, 13, 3, 2, 14, 15, 1)
KV_COPIES = 16


def nn(a, b):
    return jnp.dot(a, b, preferred_element_type=F32)


def nt(a, b):
    return lax.dot_general(a, b, (((1,), (1,)), ((), ())), preferred_element_type=F32)


def silu(v):
    return v / (1.0 + jnp.exp(-v))


def layer_kernel(
    x_h, ag_h, wq_h, wk_h, wv_h, wf_h, fb_h, wo_h, kv_h, cum_h, len_h, fg_h,
    ids_h, rw_h, sg_h, su_h, sd_h, eg_h, eu_h, ed_h,
    out_ref, nkv_ref,
    x_v, ag_v, w_v, fb_v, wo_v, kv_v, cum_v, len_v, fg_v,
    ids_v, rw_v, sg_v, su_v, sd_v, eg_v, eu_v, ed_v,
    part_s, part_r, mid_a, dsp_s, dsp_r, ret_s, ret_r, fin_s, fin_r, out_a,
    lsem, ksem, send_sem, recv_sem, ready,
):
    ep = lax.axis_index("ep")
    tp = lax.axis_index("tp")

    copies = [
        (x_h, x_v), (ag_h, ag_v),
        (wk_h, w_v.at[pl.ds(0, HEAD)]), (wv_h, w_v.at[pl.ds(HEAD, HEAD)]),
        (wq_h, w_v.at[pl.ds(2 * HEAD, HEAD)]), (wf_h, w_v.at[pl.ds(3 * HEAD, N)]),
        (fb_h, fb_v), (cum_h, cum_v), (len_h, len_v),
        (wo_h, wo_v.at[pl.ds(HEAD, HEAD)]), (ids_h, ids_v), (rw_h, rw_v), (fg_h, fg_v),
        (sg_h, sg_v), (su_h, su_v), (sd_h, sd_v), (eg_h, eg_v), (eu_h, eu_v), (ed_h, ed_v),
    ]
    local = [pltpu.make_async_copy(s, d, lsem.at[i]) for i, (s, d) in enumerate(copies)]
    per = ROWS // KV_COPIES
    cached = [
        pltpu.make_async_copy(kv_h.at[pl.ds(i * per, per)], kv_v.at[pl.ds(i * per, per)], ksem.at[i])
        for i in range(KV_COPIES)
    ]
    for c in local[:9]:
        c.start()
    for c in cached:
        c.start()
    for c in local[9:]:
        c.start()

    barrier = pltpu.get_barrier_semaphore()
    for j in range(1, N):
        pl.semaphore_signal(barrier, inc=1, device_id=(ep, lax.rem(tp + j, N)), device_id_type=MESH)
        pl.semaphore_signal(barrier, inc=1, device_id=(lax.rem(ep + j, N), tp), device_id_type=MESH)

    def all_sent(phase, ref):
        pltpu.make_async_remote_copy(
            src_ref=ref, dst_ref=ref, send_sem=send_sem.at[phase], recv_sem=recv_sem.at[phase],
            device_id=(ep, lax.rem(tp + 1, N)), device_id_type=MESH,
        ).wait_send()

    def all_arrived(phase, ref):
        pltpu.make_async_remote_copy(
            src_ref=ref, dst_ref=ref, send_sem=send_sem.at[phase], recv_sem=recv_sem.at[phase],
            device_id=(ep, lax.rem(tp + 1, N)), device_id_type=MESH,
        ).wait_recv()

    def push(phase, src, dst, device):
        pltpu.make_async_remote_copy(
            src_ref=src, dst_ref=dst, send_sem=send_sem.at[phase], recv_sem=recv_sem.at[phase],
            device_id=device, device_id_type=MESH,
        ).start()

    def scatter_tp(phase, src, dst):
        for j in TP_ORDER:
            to = lax.rem(tp + j, N)
            push(phase, src.at[to], dst.at[j - 1], (ep, to))

    def gather_tp(phase, ref):
        for j in TP_ORDER:
            push(phase, ref.at[tp], ref.at[tp], (ep, lax.rem(tp + j, N)))

    def everywhere(phase, pick, dst):
        def to_ep(i, carry):
            far = lax.rem(ep + i, N)
            for j in (0,) + TP_ORDER:
                to = lax.rem(tp + j, N)
                push(phase, pick(far, to), dst, (far, to))
            return carry

        lax.fori_loop(1, N, to_ep, 0)
        for j in TP_ORDER:
            to = lax.rem(tp + j, N)
            push(phase, pick(ep, to), dst, (ep, to))

    w_v[pl.ds(3 * HEAD + N, HEAD - N)] = jnp.zeros((HEAD - N, WIDTH), BF)
    wo_v[pl.ds(0, HEAD)] = jnp.zeros((HEAD, WIDTH), BF)

    for c in local[:7]:
        c.wait()
    wide = x_v[...].astype(F32)
    factor = lax.rsqrt(jnp.mean(wide * wide, axis=-1, keepdims=True) + NORM_EPS)
    normed = (wide * factor * ag_v[...]).astype(BF)
    res = nt(normed, w_v[...])
    nkv = res[:, :LANES].astype(BF)
    nkv_ref[...] = nkv
    nkv_f = nkv.astype(F32)
    rest = res[:, LANES:]
    lane = lax.broadcasted_iota(jnp.int32, (ROWS, LANES), 1)
    q_f = jnp.where(lane < HEAD, rest, 0.0).astype(BF).astype(F32)
    bias = jnp.sum(
        jnp.where(lax.broadcasted_iota(jnp.int32, (1, N), 1) == tp, fb_v[...], 0.0),
        axis=-1, keepdims=True,
    )
    logit = jnp.sum(jnp.where(lane == HEAD + tp, rest, 0.0), axis=-1, keepdims=True) + bias
    forget = jnp.minimum(logit, 0.0) - jnp.log(1.0 + jnp.exp(-jnp.abs(logit)))
    scaling = HEAD ** (-0.5)
    itself = jnp.sum(q_f * nkv_f, axis=-1, keepdims=True) * scaling

    local[7].wait()
    local[8].wait()
    diag = lax.broadcasted_iota(jnp.int32, (ROWS, ROWS), 0) == lax.broadcasted_iota(
        jnp.int32, (ROWS, ROWS), 1
    )
    length = jnp.sum(
        jnp.where(diag, len_v[...].astype(F32), 0.0), axis=-1, keepdims=True
    ).astype(jnp.int32)
    position = lax.broadcasted_iota(jnp.int32, (8, SPAN), 1)
    row8 = lax.broadcasted_iota(jnp.int32, (8, LANES), 0)
    pieces = []
    for g in range(ROWS // 8):
        here = slice(8 * g, 8 * g + 8)
        for c in cached[8 // per * g : 8 // per * (g + 1)]:
            c.wait()
        q8 = q_f[here]
        scores = jnp.zeros((8, SPAN), F32)
        for p in range(4):
            asked = jnp.concatenate(
                [jnp.where(row8 == 2 * p, q8, 0.0), jnp.where(row8 == 2 * p + 1, q8, 0.0)], axis=1
            ).astype(BF)
            pair = jnp.concatenate([kv_v[8 * g + 2 * p], kv_v[8 * g + 2 * p + 1]], axis=1)
            scores = scores + nt(asked, pair)
        cum = cum_v[pl.ds(8 * g, 8), 0, :]
        len8 = length[here]
        latest = jnp.sum(jnp.where(position == len8 - 1, cum, 0.0), axis=-1, keepdims=True)
        scores = scores * scaling + (latest + forget[here]) - cum
        scores = jnp.where(position < len8, scores, -jnp.inf)
        highest = jnp.maximum(jnp.max(scores, axis=-1, keepdims=True), itself[here])
        earlier = jnp.exp(scores - highest)
        own = jnp.exp(itself[here] - highest)
        denominator = jnp.sum(earlier, axis=-1, keepdims=True) + own
        probs = (earlier / denominator).astype(BF)
        att = (own / denominator).astype(BF).astype(F32) * nkv_f[here]
        for p in range(4):
            pair = jnp.concatenate([kv_v[8 * g + 2 * p], kv_v[8 * g + 2 * p + 1]], axis=1)
            o = nn(probs, pair)
            att = att + jnp.where(row8 == 2 * p, o[:, :LANES], 0.0)
            att = att + jnp.where(row8 == 2 * p + 1, o[:, LANES:], 0.0)
        pieces.append(att)
    attended = jnp.where(lane >= HEAD, jnp.concatenate(pieces, axis=0), 0.0).astype(BF)

    local[9].wait()
    head_part = nn(attended, wo_v[...]).astype(BF)
    for c in range(N):
        part_s[c] = head_part[:, c * LANES : (c + 1) * LANES]
    pl.semaphore_wait(barrier, 2 * (N - 1))
    for j in range(1, N):
        pl.semaphore_signal(
            ready, inc=1, device_id=(lax.rem(ep + j, N), tp), device_id_type=MESH
        )
    scatter_tp(0, part_s, part_r)

    for c in local[10:13]:
        c.wait()
    experts = N * N // 2
    slot = lax.broadcasted_iota(jnp.int32, (2 * experts, ROWS), 0)
    target = slot // 2
    member = jnp.zeros(slot.shape, F32)
    weight = jnp.zeros(slot.shape, F32)
    for k in range(ids_v.shape[0]):
        hit = ids_v[pl.ds(k, 1), :] == target
        member = jnp.where(hit, 1.0, member)
        weight = weight + jnp.where(hit, rw_v[pl.ds(k, 1), :], 0.0)
    before = jnp.where(
        lax.broadcasted_iota(jnp.int32, (ROWS, ROWS), 0)
        < lax.broadcasted_iota(jnp.int32, (ROWS, ROWS), 1),
        1.0,
        0.0,
    ).astype(BF)
    rank = nn(member.astype(BF), before)
    placed = (member > 0.5) & (jnp.abs(rank - (slot % 2).astype(F32)) < 0.5)
    placement = jnp.where(placed, 1.0, 0.0).astype(BF)
    shares = jnp.where(placed, weight, 0.0)
    high = shares.astype(BF)
    low = (shares - high.astype(F32)).astype(BF)
    unit = jnp.where(diag, 1.0, 0.0).astype(BF)
    high = nt(unit, high).astype(BF)
    low = nt(unit, low).astype(BF)

    all_arrived(0, part_r)
    total = part_s[tp].astype(F32)
    for j in range(N - 1):
        total = total + part_r[j].astype(F32)
    own_stream = x_v[:, pl.ds(pl.multiple_of(tp * LANES, LANES), LANES)].astype(F32)
    middle = (own_stream + total).astype(BF)
    mid_a[tp] = middle
    dsp_s.reshape(2 * experts, LANES)[...] = nn(placement, middle).astype(BF)
    pl.semaphore_wait(ready, N - 1)
    everywhere(2, lambda e, t: dsp_s.at[e * (N // 2) + t // 2], dsp_r.at[tp, ep])
    dsp_r[tp, ep] = dsp_s[ep * (N // 2) + tp // 2]
    gather_tp(1, mid_a)

    def normalised(blocks):
        square = jnp.zeros((ROWS, LANES), F32)
        for c in range(N):
            m = blocks[c].astype(F32)
            square = square + m * m
        factor = lax.rsqrt(jnp.sum(square, axis=-1, keepdims=True) * (1.0 / WIDTH) + NORM_EPS)
        return jnp.concatenate(
            [
                (blocks[c].astype(F32) * factor * fg_v[:, c * LANES : (c + 1) * LANES]).astype(BF)
                for c in range(N)
            ],
            axis=1,
        )

    for c in local[13:]:
        c.wait()
    all_arrived(2, dsp_r.reshape(N * N, 2, LANES).at[pl.ds(0, N * N - 1)])
    batch = normalised(dsp_r.reshape(N, ROWS, LANES))
    hidden = (silu(nn(batch, eg_v[...])) * nn(batch, eu_v[...])).astype(BF)
    served = nn(hidden, ed_v[...]).astype(BF)
    ret_rows = ret_s.reshape(N, ROWS, LANES)
    for c in range(N):
        ret_rows[c] = served[:, c * LANES : (c + 1) * LANES]
    mine = ep * (N // 2) + tp // 2
    everywhere(3, lambda e, t: ret_s.at[t, e], ret_r.at[lax.rem(tp, 2), mine])
    ret_r[lax.rem(tp, 2), mine] = ret_s[tp, ep]

    all_arrived(1, mid_a.at[pl.ds(0, N - 1)])
    hidden_in = normalised(mid_a)
    shared_hidden = (silu(nt(hidden_in, sg_v[...])) * nt(hidden_in, su_v[...])).astype(BF)
    mixed = nn(shared_hidden, sd_v[...]).astype(BF)
    for c in range(N):
        fin_s[c] = mixed[:, c * LANES : (c + 1) * LANES]
    scatter_tp(4, fin_s, fin_r)

    all_arrived(4, fin_r)
    total = mid_a[tp].astype(F32) + fin_s[tp].astype(F32)
    for j in range(N - 1):
        total = total + fin_r[j].astype(F32)
    all_arrived(3, ret_r.reshape(N * N, 2, LANES).at[pl.ds(0, N * N - 1)])
    ret_half = ret_r.reshape(2, 2 * experts, LANES)
    for c in range(2):
        returned = ret_half[c]
        total = total + nn(high, returned) + nn(low, returned)
    out_a[tp] = total.astype(BF)
    gather_tp(5, out_a)
    all_arrived(5, out_a.at[pl.ds(0, N - 1)])
    for c in range(N):
        out_ref[:, c * LANES : (c + 1) * LANES] = out_a[c]

    for phase in (0, 1, 4, 5):
        all_sent(phase, part_r)
    for phase in (2, 3):
        all_sent(phase, dsp_r.reshape(N * N, 2, LANES).at[pl.ds(0, N * N - 1)])


def body(
    layer_in, attn_gain, query_weight, key_weight, value_weight, forget_weight, forget_bias,
    out_weight, kv_cache, cum_gates, lengths, ffn_gain, route_ids, route_weights,
    shared_gate, shared_up, shared_down, expert_gate, expert_up, expert_down,
):
    operands = (
        layer_in, attn_gain.reshape(1, -1), query_weight.T, key_weight.T, value_weight.T,
        forget_weight.T, forget_bias.reshape(1, -1), out_weight, kv_cache[:, 0], cum_gates,
        lengths.reshape(1, -1), ffn_gain.reshape(1, -1), route_ids.T, route_weights.T,
        shared_gate.T, shared_up.T, shared_down, expert_gate[0], expert_up[0], expert_down[0],
    )
    picks = route_ids.shape[1]
    block = (N, ROWS, LANES)
    layer_out, new_kv = pl.pallas_call(
        layer_kernel,
        out_shape=(
            pltpu.VMEM((ROWS, WIDTH), BF),
            pltpu.VMEM((ROWS, LANES), BF),
        ),
        in_specs=[pl.BlockSpec(memory_space=pltpu.HBM)] * len(operands),
        out_specs=[pl.BlockSpec(memory_space=pltpu.VMEM)] * 2,
        scratch_shapes=[
            pltpu.VMEM((ROWS, WIDTH), BF),
            pltpu.VMEM((1, WIDTH), F32),
            pltpu.VMEM((4 * HEAD, WIDTH), BF),
            pltpu.VMEM((1, N), F32),
            pltpu.VMEM((2 * HEAD, WIDTH), BF),
            pltpu.VMEM((ROWS, SPAN, LANES), BF),
            pltpu.VMEM((ROWS, 1, SPAN), F32),
            pltpu.VMEM((1, ROWS), jnp.int32),
            pltpu.VMEM((1, WIDTH), F32),
            pltpu.VMEM((picks, ROWS), jnp.int32),
            pltpu.VMEM((picks, ROWS), F32),
            pltpu.VMEM((ROWS, WIDTH), BF),
            pltpu.VMEM((ROWS, WIDTH), BF),
            pltpu.VMEM((ROWS, WIDTH), BF),
            pltpu.VMEM((WIDTH, 4 * HEAD), BF),
            pltpu.VMEM((WIDTH, 4 * HEAD), BF),
            pltpu.VMEM((4 * HEAD, WIDTH), BF),
            pltpu.VMEM(block, BF),
            pltpu.VMEM((N - 1, ROWS, LANES), BF),
            pltpu.VMEM(block, BF),
            pltpu.VMEM((N * N // 2, 2, LANES), BF),
            pltpu.VMEM((N, N, 2, LANES), BF),
            pltpu.VMEM((N, N, 2, LANES), BF),
            pltpu.VMEM((2, N * N // 2, 2, LANES), BF),
            pltpu.VMEM(block, BF),
            pltpu.VMEM((N - 1, ROWS, LANES), BF),
            pltpu.VMEM(block, BF),
            pltpu.SemaphoreType.DMA((len(operands) - 1,)),
            pltpu.SemaphoreType.DMA((KV_COPIES,)),
            pltpu.SemaphoreType.DMA((6,)),
            pltpu.SemaphoreType.DMA((6,)),
            pltpu.SemaphoreType.REGULAR,
        ],
        compiler_params=pltpu.CompilerParams(collective_id=0, has_side_effects=True),
        name="decode_layer",
    )(*operands)
    return (layer_out, new_kv[:, None, :])


def solution(mesh):
    placed = (
        P("ep", None), P(), P(None, "tp"), P(None, "tp"), P(None, "tp"), P(), P(), P("tp", None),
        P("ep", "tp", None, None), P("ep", "tp", None), P("ep"), P(), P("ep", None),
        P("ep", None), P(None, "tp"), P(None, "tp"), P("tp", None), P(("ep", "tp"), None, None),
        P(("ep", "tp"), None, None), P(("ep", "tp"), None, None),
    )
    return jax.shard_map(
        body,
        mesh=mesh,
        in_specs=placed,
        out_specs=(P("ep", None), P("ep", "tp", None)),
        check_vma=False,
    )
```
